32 devices in a mesh: rep: 2 (over x), fs: 8 (over z, y), tp: 2 (over core).
Axes of the slice: x: 2, y: 2, z: 4, core: 2. Of those that a mesh axis runs over, the one named last changes fastest.
Arguments:
- tokens: bfloat16 [12288, 2048], P(('rep', 'fs', 'tp')), may hold values from -6 to 6
- norm_gain: float32 [2048], replicated, may hold values from 0.1 to 1.9
- gate_weight: float32 [2048, 5632], P('fs', 'tp'), may hold values from -0.125 to 0.125
- up_weight: float32 [2048, 5632], P('fs', 'tp'), may hold values from -0.125 to 0.125
- gate_scale: float32 [5632], P('tp'), may hold values from 0.3 to 3
- up_scale: float32 [5632], P('tp'), may hold values from 0.3 to 3
- down_weight: float32 [5632, 2048], P('tp', 'fs'), may hold values from -0.078125 to 0.078125
- down_scale: float32 [2048], replicated, may hold values from 0.3 to 3
Outputs:
- mixed: bfloat16 [12288, 2048], P(('rep', 'fs', 'tp'))
The draws below stay inside these ranges and needn't reach their ends.
All inputs are finite; a program needn't handle non-finite values.
Results may differ from the reference program's by a relative error of at most 0.014.
Values may be sent and summed in bfloat16 or wider, within the bound.
A program may use at most 128 MiB of HBM per device.

```python
import math
import jax
import jax.numpy as jnp
from jax import lax

D = 2048
FF = 5632
TOKENS = 12288
N_TP = 2


def level_of(own_key, dims, pieces, smallest, largest):
    def one(axis_at, blocks):
        steps = jax.random.uniform(jax.random.fold_in(jax.random.fold_in(own_key, 6), axis_at), (blocks,), jnp.float32, smallest / len(pieces), largest / len(pieces))
        return jnp.repeat(jnp.exp(steps), dims[axis_at] // blocks).reshape((-1,) + (1,) * (len(dims) - axis_at - 1))

    level = one(*pieces[0])
    for cut in pieces[1:]:
        level = level * one(*cut)
    return level


def gaussian(key, extent, scale, bound, cuts=(), held_as=jnp.bfloat16):
    drawn = scale * jax.random.normal(key, extent, jnp.float32)
    if cuts:
        drawn = drawn * level_of(key, extent, cuts, -0.22, 0.18)
    return jnp.clip(drawn, -bound, bound).astype(held_as)


def setup_inputs(seed: int = 0) -> dict:
    splits = jax.random.split(jax.random.key(seed), 9)
    tokens = gaussian(splits[0], (TOKENS, D), 1.0, 6.0, ((0, 32),))
    norm_gain = jnp.clip(1.0 + 0.18 * jax.random.normal(splits[1], (D,), jnp.float32), 0.1, 1.9)
    gate_weight = gaussian(splits[2], (D, FF), D ** -0.5, 0.125, ((0, 8), (1, 2)), jnp.float32)
    up_weight = gaussian(splits[3], (D, FF), D ** -0.5, 0.125, ((0, 8), (1, 2)), jnp.float32)
    gate_scale = jnp.clip(jnp.exp(math.log(3.0) - 2.3025851 * jax.random.uniform(splits[4], (FF,), jnp.float32) ** level_of(splits[4], (FF,), ((0, 2),), -0.2, 0.2)), 0.3, 3.0)
    up_scale = jnp.clip(jnp.exp(math.log(3.0) - 2.3025851 * jax.random.uniform(splits[5], (FF,), jnp.float32) ** level_of(splits[5], (FF,), ((0, 2),), -0.2, 0.2)), 0.3, 3.0)
    down_weight = gaussian(splits[6], (FF, D), FF ** -0.5, 0.078125, ((0, 2), (1, 8)), jnp.float32)
    down_scale = jnp.clip(jnp.exp(jax.random.uniform(splits[7], (D,), jnp.float32, math.log(0.3), math.log(3.0))), 0.3, 3.0)
    return {"tokens": tokens, "norm_gain": norm_gain, "gate_weight": gate_weight, "up_weight": up_weight, "gate_scale": gate_scale, "up_scale": up_scale, "down_weight": down_weight, "down_scale": down_scale}


def reference(tokens, norm_gain, gate_weight, up_weight, gate_scale, up_scale, down_weight, down_scale):
    values = tokens.astype(jnp.float32)
    normed = (values * lax.rsqrt(lax.optimization_barrier(jnp.mean(values * values, axis=-1, keepdims=True)) + 1e-06) * norm_gain).astype(jnp.bfloat16)
    block_width = FF // N_TP
    gate_blocks = gate_weight.astype(jnp.bfloat16).reshape(D, N_TP, block_width).transpose(1, 0, 2)
    up_blocks = up_weight.astype(jnp.bfloat16).reshape(D, N_TP, block_width).transpose(1, 0, 2)
    down_blocks = down_weight.astype(jnp.bfloat16).reshape(N_TP, block_width, D)
    gate_scales = gate_scale.reshape(N_TP, block_width)
    up_scales = up_scale.reshape(N_TP, block_width)

    def one_block(running, blocks):
        gate_piece, up_piece, gate_factor, up_factor, down_piece = blocks
        gate_value = jnp.dot(normed, gate_piece, preferred_element_type=jnp.float32) * gate_factor
        up_value = jnp.dot(normed, up_piece, preferred_element_type=jnp.float32) * up_factor
        hidden = (jax.nn.silu(gate_value) * up_value).astype(jnp.bfloat16)
        partial_value = jnp.dot(hidden, down_piece, preferred_element_type=jnp.float32).astype(jnp.bfloat16)
        return (running + partial_value.astype(jnp.float32), None)
    summed, unused = lax.scan(one_block, jnp.zeros((tokens.shape[0], D), jnp.float32), (gate_blocks, up_blocks, gate_scales, up_scales, down_blocks))
    return (summed * down_scale).astype(jnp.bfloat16)
```

```python
import functools
import math

import jax
import jax.numpy as jnp
from jax import lax
from jax.experimental import pallas as pl
from jax.experimental.pallas import tpu as pltpu
from jax.sharding import PartitionSpec as P


def grid_of(count):
    inner = 1
    while (inner * 2) ** 2 <= count and count % (inner * 2) == 0:
        inner *= 2
    return count // inner, inner


def swap(x, axis):
    return lax.ppermute(x, axis, [(0, 1), (1, 0)])


def gather_kernel(outer, inner, *refs):
    local, whole = refs[:3], refs[3:6]
    own_sem, near_sem, relay_sem, cross_sem, recv_sem = refs[6:]
    me = lax.axis_index("fs")
    z, y = me // inner, lax.rem(me, inner)
    offsets = [o for o in (1, -1, 2, -2) if abs(o) < outer]

    def inside(o):
        return (z + o >= 0) & (z + o < outer)

    def peer(i):
        return z * inner + lax.rem(y + i, inner)

    barrier = pltpu.get_barrier_semaphore()
    for o in offsets:

        @pl.when(inside(o))
        def _():
            pl.semaphore_signal(
                barrier, inc=1, device_id={"fs": me + o * inner},
                device_id_type=pl.DeviceIdType.MESH,
            )

    for i in range(1, inner):
        pl.semaphore_signal(
            barrier, inc=1, device_id={"fs": peer(i)}, device_id_type=pl.DeviceIdType.MESH
        )
    reach = min(2, outer - 1)
    peers = jnp.minimum(z, reach) + jnp.minimum(outer - 1 - z, reach) + inner - 1
    pl.semaphore_wait(barrier, peers)

    def slot(a, row, column):
        return row * inner + column if a < 2 else row

    def send(a, source, row, column, target, sem):
        place = slot(a, row, column)
        return pltpu.make_async_remote_copy(
            src_ref=source,
            dst_ref=whole[a].at[place],
            send_sem=sem,
            recv_sem=recv_sem.at[a, place],
            device_id={"fs": target},
            device_id_type=pl.DeviceIdType.MESH,
        )

    def near(a, o):
        return send(a, local[a], z, y, me + o * inner, near_sem.at[a, offsets.index(o)])

    def relay(a, d):
        step = 1 if d > 0 else -1
        source = whole[a].at[slot(a, z - d, y)]
        return send(a, source, z - d, y, me + step * inner, relay_sem.at[a, outer + d])

    def cross(a, d, i):
        source = local[a] if d == 0 else whole[a].at[slot(a, z - d, y)]
        return send(a, source, z - d, y, peer(i), cross_sem.at[a, outer + d, i])

    def arrived(a, row, column):
        place = slot(a, row, column)
        return pltpu.make_async_copy(local[a], whole[a].at[place], recv_sem.at[a, place])

    def keep(a):
        return pltpu.make_async_copy(local[a], whole[a].at[slot(a, z, y)], own_sem.at[a])

    def take(a, d):
        @pl.when(inside(-d))
        def _():
            arrived(a, z - d, y).wait()
            if a < 2:
                for i in range(1, inner):
                    cross(a, d, i).start()
            if abs(d) >= 2:
                step = 1 if d > 0 else -1

                @pl.when(inside(step))
                def _():
                    relay(a, d).start()

    def open_near(a, o):
        @pl.when(inside(o))
        def _():
            near(a, o).start()

    distances = [d * sign for d in range(1, outer) for sign in (1, -1)]
    for o in offsets[:2]:
        open_near(0, o)
    for i in range(1, inner):
        cross(0, 0, i).start()
    for o in offsets[:2]:
        open_near(1, o)
    for i in range(1, inner):
        cross(1, 0, i).start()
    for a in range(2):
        for o in offsets[2:]:
            open_near(a, o)
    for a in range(3):
        keep(a).start()
    for d in distances[:4]:
        for a in range(2):
            take(a, d)
    for o in offsets:
        open_near(2, o)
    for d in distances[4:]:
        for a in range(2):
            take(a, d)
    for d in distances:
        take(2, d)

    for a in range(3):
        keep(a).wait()
        for o in offsets:

            @pl.when(inside(o))
            def _():
                near(a, o).wait_send()

        for d in distances:
            if abs(d) >= 2:

                @pl.when(inside(-d) & inside(1 if d > 0 else -1))
                def _():
                    relay(a, d).wait_send()

    for a in range(2):
        for d in [0] + distances:

            @pl.when(inside(-d))
            def _():
                for i in range(1, inner):
                    cross(a, d, i).wait_send()
                    arrived(a, z - d, lax.rem(y + i, inner)).wait()


def gather_weights(outer, inner, gate, up, down):
    shapes = [(outer * inner, *gate.shape), (outer * inner, *up.shape), (outer, *down.shape)]
    anywhere = pl.BlockSpec(memory_space=pl.ANY)
    return pl.pallas_call(
        functools.partial(gather_kernel, outer, inner),
        out_shape=[jax.ShapeDtypeStruct(shape, gate.dtype) for shape in shapes],
        in_specs=[anywhere] * 3,
        out_specs=[anywhere] * 3,
        scratch_shapes=[
            pltpu.SemaphoreType.DMA((3,)),
            pltpu.SemaphoreType.DMA((3, 4)),
            pltpu.SemaphoreType.DMA((3, 2 * outer)),
            pltpu.SemaphoreType.DMA((2, 2 * outer, inner)),
            pltpu.SemaphoreType.DMA((3, outer * inner)),
        ],
        compiler_params=pltpu.CompilerParams(collective_id=0, has_side_effects=True),
        cost_estimate=pl.CostEstimate(
            flops=0, bytes_accessed=32 * sum(math.prod(shape) for shape in shapes), transcendentals=0
        ),
    )(gate, up, down)


def roll(x, shift):
    return lax.dynamic_slice_in_dim(jnp.concatenate([x, x], -1), shift, x.shape[-1], x.ndim - 1)


def reorder(x, outer, inner, y):
    block = x.shape[-1] // (outer * inner)
    position = lax.broadcasted_iota(jnp.int32, x.shape, x.ndim - 1) % (inner * block)
    ahead = roll(x, y * block)
    behind = roll(x, (x.shape[-1] - inner * block + y * block) % x.shape[-1])
    return jnp.where(position + y * block < inner * block, ahead, behind)


def gather_rows(x, axis):
    if lax.axis_size(axis) == 2:
        return jnp.stack([x, swap(x, axis)])
    return lax.all_gather(x, axis)


def reduce_rows(x, axis):
    if lax.axis_size(axis) == 2:
        return x[0].astype(jnp.float32) + swap(x[1].astype(jnp.bfloat16), axis).astype(jnp.float32)
    return lax.psum_scatter(
        x.astype(jnp.bfloat16), axis, scatter_dimension=0, tiled=False
    ).astype(jnp.float32)


def on_device(
    tokens, norm_gain, gate_weight, up_weight, gate_scale, up_scale, down_weight, down_scale
):
    groups, count = lax.axis_size("rep"), lax.axis_size("fs")
    tps = lax.axis_size("tp")
    outer, inner = grid_of(count)
    y = lax.axis_index("fs") % inner
    width = gate_weight.shape[1] // groups
    start = lax.axis_index("rep") * width
    gate_local, up_local = (
        lax.dynamic_slice_in_dim(weight, start, width, 1).astype(jnp.bfloat16)
        for weight in (gate_weight, up_weight)
    )
    down_local = lax.dynamic_slice_in_dim(down_weight, start, width, 0).astype(jnp.bfloat16)
    gate_scale, up_scale = (
        lax.dynamic_slice_in_dim(scale, start, width, 0) for scale in (gate_scale, up_scale)
    )

    gate_whole, up_whole, down_near = gather_weights(
        outer, inner, gate_local, up_local, down_local
    )

    values = tokens.astype(jnp.float32)
    own_normed = (
        values * lax.rsqrt(jnp.mean(values * values, axis=-1, keepdims=True) + 1e-06) * norm_gain
    ).astype(jnp.bfloat16)
    rows, depth = own_normed.shape
    normed = gather_rows(gather_rows(own_normed, "tp"), "rep").swapaxes(0, 1).reshape(-1, depth)

    gate_whole, up_whole = gate_whole.reshape(depth, width), up_whole.reshape(depth, width)
    cuts = [slice(0, outer // 2), slice(outer // 2, outer)] if outer > 1 else [slice(0, 1)]
    pieces = [down_near[cut] for cut in cuts]
    for i in range(1, inner):
        pairs = [(f, f - f % inner + (f - i) % inner) for f in range(count)]
        pieces += [lax.ppermute(down_near[cut], "fs", pairs) for cut in cuts]
    gate_value = jnp.dot(normed, gate_whole, preferred_element_type=jnp.float32)
    up_value = jnp.dot(normed, up_whole, preferred_element_type=jnp.float32)
    hidden = (jax.nn.silu(gate_value * gate_scale) * (up_value * up_scale)).astype(jnp.bfloat16)

    near = len(cuts)
    later, pieces[near:] = lax.optimization_barrier((hidden, pieces[near:]))
    block = down_local.shape[1]
    columns = []
    for at, piece in enumerate(pieces):
        partial_value = jnp.dot(
            hidden if at < near else later, jnp.concatenate(list(piece), 1), preferred_element_type=jnp.float32
        ).astype(jnp.bfloat16)
        partial_value = partial_value.reshape(tps, groups, rows, -1)
        total = reduce_rows(reduce_rows(partial_value, "tp"), "rep")
        columns += [total[:, c * block : (c + 1) * block] for c in range(len(piece))]
    summed = jnp.concatenate([columns[i * outer + a] for a in range(outer) for i in range(inner)], -1)
    scale = reorder(down_scale[None], outer, inner, y)
    mixed = (summed * scale).astype(jnp.bfloat16)
    return reorder(mixed, outer, inner, (inner - y) % inner)


def solution(mesh):
    placed = (
        P(("rep", "fs", "tp"), None),
        P(),
        P("fs", "tp"),
        P("fs", "tp"),
        P("tp"),
        P("tp"),
        P("tp", "fs"),
        P(),
    )
    return jax.shard_map(
        on_device,
        mesh=mesh,
        in_specs=placed,
        out_specs=P(("rep", "fs", "tp"), None),
        check_vma=False,
    )
```
